256 devices in a mesh: sp: 32 (over z, x), tp: 8 (over y, core).
Axes of the slice: x: 4, y: 4, z: 8, core: 2. Of those that a mesh axis runs over, the one named last changes fastest.
Arguments:
- tokens: bfloat16 [16384, 2048], P(('sp', 'tp')), may hold values from -6 to 6
- norm_gain: float32 [2048], replicated, may hold values from 0.1 to 1.9
- w_query: bfloat16 [2048, 1024], P(None, 'tp'), may hold values from -16 to 16
- w_key: bfloat16 [2048, 1024], P(None, 'tp'), may hold values from -16 to 16
- w_value: bfloat16 [2048, 1024], P(None, 'tp'), may hold values from -0.125 to 0.125
- conv_in: bfloat16 [2048, 2048], P(None, 'tp'), may hold values from -0.125 to 0.125
- conv_gate: bfloat16 [2048, 2048], P(None, 'tp'), may hold values from -0.125 to 0.125
- conv_taps: float32 [31, 2048], P(None, 'tp'), may hold values from -3.7 to 3.7
- conv_gain: float32 [2048], P('tp'), may hold values from 0.1 to 1.9
- cum_gate: float32 [16, 16384], P('tp'), may hold values from -2050 to 0, as said below
- out_attn: bfloat16 [1024, 2048], P('tp'), may hold values from -0.75 to 0.75
- out_conv: bfloat16 [2048, 2048], P('tp'), may hold values from -0.125 to 0.125
Outputs:
- mixed: bfloat16 [16384, 2048], P(('sp', 'tp'))
- log_total: float32 [16, 16384], P('tp', 'sp')
The draws below stay inside these ranges and needn't reach their ends.
Inputs may be any that keep to these rules, and one draw needn't show every extreme that they name: `cum_gate`: for each head the values never rise from one position to the next and are at most 0.
All inputs are finite; a program needn't handle non-finite values.
Results may differ from the reference program's by a relative error of at most 0.014.
Values may be sent and summed in bfloat16 or wider, within the bound.
No kernel may reach another device: no remote copies, remote signals or barrier semaphores. Data moves between devices by JAX's collectives and lax.ppermute only.
A program may use at most 128 MiB of HBM per device.

```python
import math
import jax
import jax.numpy as jnp
from jax import lax

D = 2048
HEAD_COUNT = 16
HEAD = 64
KERNEL = 31
TOK_DEV = 512
TOKEN_COUNT = 16384
ATT_WIDTH = 1024
CONV = 2048
N_SP = 32
N_TP = 8


def query_key_pair(key):
    random_split_keys = jax.random.split(jax.random.fold_in(key, 11), 3)
    fan_scale = D ** (-0.5)
    key_weight = jnp.clip(jax.random.normal(random_split_keys[0], (D, HEAD_COUNT * HEAD), jnp.float32), -6.0, 6.0) * fan_scale
    query_weight = jnp.clip(jax.random.normal(random_split_keys[2], (D, HEAD_COUNT * HEAD), jnp.float32), -6.0, 6.0) * (2.25 * fan_scale)
    return (query_weight, key_weight)


def draw_w_query(key, part):
    return query_key_pair(key)[0].astype(jnp.bfloat16)


def draw_w_key(key, part):
    return query_key_pair(key)[1].astype(jnp.bfloat16)


def draw_conv_taps(key, part):
    random_split_keys = jax.random.split(jax.random.fold_in(key, 23), 1)
    sequence_positions = jnp.arange(CONV, dtype=jnp.float32) / (CONV - 1)
    raw_taps = jnp.clip(jax.random.normal(random_split_keys[0], (KERNEL, CONV), jnp.float32), -4.0, 4.0)
    channel_ramp = 10.0 ** (sequence_positions - 0.5)
    return raw_taps * KERNEL ** (-0.5) * channel_ramp[None, :]


def draw_cum_gate(key, part):
    random_split_keys = jax.random.split(jax.random.fold_in(key, 37), 7)
    head_order = jax.random.permutation(random_split_keys[0], HEAD_COUNT)
    slow_count = HEAD_COUNT // 2
    slow_heads = (head_order < slow_count)[:, None]
    slow_total = jax.random.uniform(random_split_keys[1], (HEAD_COUNT, 1), jnp.float32, 0.5, 1.0)
    fast_rate = 1.0 / jax.random.uniform(random_split_keys[2], (HEAD_COUNT, 1), jnp.float32, 30.0, 100.0)
    baseline_forget_rate = jnp.where(slow_heads, slow_total / TOKEN_COUNT, fast_rate)
    block_multiplier = jnp.exp(jax.random.uniform(random_split_keys[3], (HEAD_COUNT, N_SP), jnp.float32, math.log(0.5), math.log(2.0)))
    block_multiplier = jnp.repeat(block_multiplier, TOK_DEV, axis=1)
    roughness_multiplier = jax.random.uniform(random_split_keys[4], (HEAD_COUNT, TOKEN_COUNT), jnp.float32, 0.2, 1.8)
    spike_location = jax.random.randint(random_split_keys[5], (HEAD_COUNT, 2), 0, TOKEN_COUNT)
    spike_penalty = -jnp.log(jax.random.uniform(random_split_keys[6], (HEAD_COUNT, 2), jnp.float32, 0.6, 0.8))
    sequence_positions = jnp.arange(TOKEN_COUNT, dtype=jnp.int32)
    spike_events = jnp.sum(jnp.where(sequence_positions[None, None, :] == spike_location[:, :, None], spike_penalty[:, :, None], 0.0), axis=1)
    forget_rate_grid = baseline_forget_rate * block_multiplier * roughness_multiplier + spike_events
    return -jnp.cumsum(forget_rate_grid, axis=1)


def shard_levels(rng, dims, cuts, low, largest):
    gain = 1.0
    for axis_at, shards_of in cuts:
        draws = jax.random.uniform(jax.random.fold_in(jax.random.fold_in(rng, 6), axis_at), (shards_of,), jnp.float32, low / len(cuts), largest / len(cuts))
        gain = gain * jnp.repeat(jnp.exp(draws), dims[axis_at] // shards_of).reshape((-1,) + (1,) * (len(dims) - 1 - axis_at))
    return gain


def centred(key, dims, scale, bound, cuts=(), kind=jnp.bfloat16):
    drawn = scale * jax.random.normal(key, dims, jnp.float32)
    if cuts:
        drawn = drawn * shard_levels(key, dims, cuts, -0.22, 0.18)
    return jnp.clip(drawn, -bound, bound).astype(kind)


def setup_inputs(seed: int = 0) -> dict:
    seeds = jax.random.split(jax.random.key(seed), 13)
    tokens = centred(seeds[0], (TOKEN_COUNT, D), 1.0, 6.0, ((0, 256),))
    norm_gain = jnp.clip(1.0 + 0.18 * jax.random.normal(seeds[1], (D,), jnp.float32), 0.1, 1.9)
    w_query = draw_w_query(jax.random.fold_in(seeds[12], 71), 0)
    w_key = draw_w_key(jax.random.fold_in(seeds[12], 71), 0)
    w_value = centred(seeds[4], (D, ATT_WIDTH), D ** -0.5, 0.125, ((1, 8),))
    conv_in = centred(seeds[5], (D, CONV), D ** -0.5, 0.125, ((1, 8),))
    conv_gate = centred(seeds[6], (D, CONV), D ** -0.5, 0.125, ((1, 8),))
    conv_taps = draw_conv_taps(jax.random.fold_in(seeds[12], 71), 0)
    conv_gain = jnp.clip(1.0 + 0.18 * jax.random.normal(seeds[8], (CONV,), jnp.float32), 0.1, 1.9)
    cum_gate = draw_cum_gate(jax.random.fold_in(seeds[12], 71), 0)
    out_attn = centred(seeds[10], (ATT_WIDTH, D), (ATT_WIDTH // 16) ** -0.5, 0.75, ((0, 8),))
    out_conv = centred(seeds[11], (CONV, D), CONV ** -0.5, 0.125, ((0, 8),))
    return dict(tokens=tokens, norm_gain=norm_gain, w_query=w_query, w_key=w_key, w_value=w_value, conv_in=conv_in, conv_gate=conv_gate, conv_taps=conv_taps, conv_gain=conv_gain, cum_gate=cum_gate, out_attn=out_attn, out_conv=out_conv)


def by_heads(matrix):
    return matrix.reshape(TOKEN_COUNT, HEAD_COUNT, HEAD).transpose(1, 0, 2)

def head_attention(operands):
    query_head, key_head, value_head, cum_head = operands
    key_place = jnp.arange(TOKEN_COUNT, dtype=jnp.int32)

    def one_block(block_index):
        begin_row = (block_index * TOK_DEV).astype(jnp.int32)
        query_block = lax.dynamic_slice_in_dim(query_head, begin_row, TOK_DEV, 0)
        cum_block = lax.dynamic_slice_in_dim(cum_head, begin_row, TOK_DEV, 0)
        query_place = begin_row + jnp.arange(TOK_DEV, dtype=jnp.int32)
        scores = jnp.dot(query_block, key_head.T, preferred_element_type=jnp.float32)
        scores = scores + cum_block[:, None] - cum_head[None, :]
        visible = key_place[None, :] <= query_place[:, None]
        scores = jnp.where(visible, scores, -1e+30)
        row_max = lax.optimization_barrier(jnp.max(scores, axis=1))
        weights = jnp.where(visible, jnp.exp(scores - row_max[:, None]), 0.0)
        row_sum = lax.optimization_barrier(jnp.sum(weights, axis=1))
        result = jnp.dot(weights.astype(jnp.bfloat16), value_head, preferred_element_type=jnp.float32)
        result = (result / row_sum[:, None]).astype(jnp.bfloat16)
        return (result, row_max + jnp.log(row_sum))
    blocks_out, totals = lax.map(one_block, jnp.arange(N_SP, dtype=jnp.int32))
    return (blocks_out.reshape(TOKEN_COUNT, HEAD), totals.reshape(TOKEN_COUNT))

def reference(tokens, norm_gain, w_query, w_key, w_value, conv_in, conv_gate, conv_taps, conv_gain, cum_gate, out_attn, out_conv):
    wide = tokens.astype(jnp.float32)
    normed = (wide * lax.rsqrt(lax.optimization_barrier(jnp.mean(wide * wide, axis=1, keepdims=True)) + 1e-06) * norm_gain[None, :]).astype(jnp.bfloat16)
    query = (jnp.dot(normed, w_query, preferred_element_type=jnp.float32) * HEAD ** (-0.5)).astype(jnp.bfloat16)
    keyed = jnp.dot(normed, w_key, preferred_element_type=jnp.float32).astype(jnp.bfloat16)
    valued = jnp.dot(normed, w_value, preferred_element_type=jnp.float32).astype(jnp.bfloat16)
    attended, log_total = lax.map(head_attention, (by_heads(query), by_heads(keyed), by_heads(valued), cum_gate))
    attended = attended.transpose(1, 0, 2).reshape(TOKEN_COUNT, ATT_WIDTH)
    opened = jnp.dot(normed, conv_in, preferred_element_type=jnp.float32)
    gating = jnp.dot(normed, conv_gate, preferred_element_type=jnp.float32)
    gated = (opened * jax.nn.sigmoid(gating)).astype(jnp.bfloat16)
    padded = jnp.concatenate([jnp.zeros((KERNEL - 1, CONV), jnp.bfloat16), gated], axis=0).astype(jnp.float32)
    convolved = jnp.zeros((TOKEN_COUNT, CONV), jnp.float32)
    for tap_index in range(KERNEL):
        convolved = convolved + conv_taps[tap_index][None, :] * padded[tap_index:tap_index + TOKEN_COUNT]
    channel_square = lax.optimization_barrier(jnp.mean(convolved * convolved, axis=1, keepdims=True))
    conv_out = jax.nn.silu(convolved * lax.rsqrt(channel_square + 1e-06) * conv_gain[None, :]).astype(jnp.bfloat16)
    group_att = ATT_WIDTH // N_TP
    group_conv = CONV // N_TP
    mixed = jnp.zeros((TOKEN_COUNT, D), jnp.float32)
    for group in range(N_TP):
        group_part = jnp.dot(attended[:, group * group_att:(group + 1) * group_att], out_attn[group * group_att:(group + 1) * group_att], preferred_element_type=jnp.float32)
        group_part = group_part + jnp.dot(conv_out[:, group * group_conv:(group + 1) * group_conv], out_conv[group * group_conv:(group + 1) * group_conv], preferred_element_type=jnp.float32)
        group_part = lax.optimization_barrier(group_part.astype(jnp.bfloat16)).astype(jnp.float32)
        mixed = mixed + group_part
    return (mixed.astype(jnp.bfloat16), log_total)
```

```python
import math

import jax
import jax.numpy as jnp
from jax import lax
from jax.experimental import pallas as pl
from jax.experimental.pallas import tpu as pltpu
from jax.sharding import Mesh, PartitionSpec as P

HEAD = 64
LOG2E = math.log2(math.e)
LN2 = math.log(2.0)
NEG = -1e30
F32 = jnp.float32
BF16 = jnp.bfloat16
VMEM = pltpu.MemorySpace.VMEM
SMEM = pltpu.MemorySpace.SMEM


def vspec():
    return pl.BlockSpec(memory_space=VMEM)


def sspec():
    return pl.BlockSpec(memory_space=SMEM)


def turn(array, axis, by):
    n = lax.axis_size(axis)
    return lax.ppermute(array, axis, [(i, (i + by) % n) for i in range(n)])


def turn_both(array, by):
    pairs = [
        (2 * y + c, 2 * ((y + by) % 4) + 1 - c) for y in range(4) for c in range(2)
    ]
    return lax.ppermute(array, ("y", "c"), pairs)


def after(x, other):
    return lax.optimization_barrier((x, other))[0]


def project_body(
    place, n0, n1, n2, n3, p0, p1, p2, p3, wq, wk, wv, wi, wg, q_out, kv_out, gated_out, xs
):
    y = place[0]
    c = place[1]
    for k, (own, other) in enumerate(((n0, p0), (n1, p1), (n2, p2), (n3, p3))):
        at = lax.rem(y + 4 - k, 4) * 128
        xs[pl.ds(pl.multiple_of(at + c * 64, 64), 64), :] = own[...]
        xs[pl.ds(pl.multiple_of(at + (1 - c) * 64, 64), 64), :] = other[...]
    x = xs[...]
    qk = jnp.dot(x, jnp.concatenate([wq[...], wk[...]], axis=1), preferred_element_type=F32)
    q_out[...] = jnp.transpose(qk[:, :128] * (LOG2E * HEAD**-0.5)).astype(BF16)
    kv_out[:512, :] = qk[:, 128:].astype(BF16)
    v = jnp.transpose(jnp.dot(x, wv[...], preferred_element_type=F32)).astype(BF16)
    for j in range(4):
        kv_out[512 + 128 * j : 640 + 128 * j, :] = v[:, 128 * j : 128 * j + 128]
    opened = jnp.dot(x, wi[...], preferred_element_type=F32)
    gating = jnp.dot(x, wg[...], preferred_element_type=F32)
    gated_out[...] = (opened * jax.nn.sigmoid(gating)).astype(BF16)


def project(place, pieces, weights):
    return pl.pallas_call(
        project_body,
        out_shape=(
            jax.ShapeDtypeStruct((128, 512), BF16),
            jax.ShapeDtypeStruct((1024, 128), BF16),
            jax.ShapeDtypeStruct((512, 256), BF16),
        ),
        in_specs=[sspec()] + [vspec()] * 13,
        out_specs=(vspec(),) * 3,
        scratch_shapes=[pltpu.VMEM((512, 2048), BF16)],
        name="project",
    )(place, *pieces, *weights)


def tile_update(h, lo, qT, kv, bias, acc, best, slot, keys, diag):
    q = qT[slot, h * HEAD : (h + 1) * HEAD, lo : lo + 256]
    zero = jnp.zeros((HEAD, 256), BF16)
    row = lax.broadcasted_iota(jnp.int32, (128, 256), 0)
    pick = jnp.where((row >= 3 * h) & (row < 3 * h + 3), 1.0, 0.0).astype(BF16)
    rhs = jnp.concatenate([q, zero, pick] if h == 0 else [zero, q, pick], axis=0)
    lhs = jnp.concatenate([kv[:keys, :], bias[:keys, :]], axis=1)
    s = jnp.dot(lhs, rhs, preferred_element_type=F32)
    if diag:
        kk = lax.broadcasted_iota(jnp.int32, (keys, 256), 0)
        qq = lax.broadcasted_iota(jnp.int32, (keys, 256), 1) + lo
        s = jnp.where(kk <= qq, s, NEG)
    old = best[slot, h, :, lo : lo + 256]
    new = jnp.maximum(old, jnp.max(s, axis=0, keepdims=True))
    p = jnp.exp2(s - new).astype(BF16)
    vT = jnp.concatenate(
        [
            kv[512 + 128 * j + h * HEAD : 512 + 128 * j + (h + 1) * HEAD, :]
            for j in range(keys // 128)
        ],
        axis=1,
    )
    vT = jnp.concatenate([vT, jnp.ones((16, keys), BF16)], axis=0)
    pv = jnp.dot(vT, p, preferred_element_type=F32)
    best[slot, h, :, lo : lo + 256] = new
    acc[slot, h, :, lo : lo + 256] = (
        acc[slot, h, :, lo : lo + 256] * jnp.exp2(old - new) + pv
    )


def whole_block(qT, kv, bias, acc, best, slot):
    for h in range(2):
        for lo in (0, 256):
            tile_update(h, lo, qT, kv, bias, acc, best, slot, 512, False)


def first_body(place, qT, kv, bias, acc, best):
    z = place[2]
    x = place[3]
    acc[...] = jnp.zeros(acc.shape, F32)
    best[...] = jnp.full(best.shape, NEG, F32)
    own = bias.at[z]
    for h in range(2):
        tile_update(h, 0, qT, kv, own, acc, best, 0, 256, True)
        tile_update(h, 256, qT, kv, own, acc, best, 0, 512, True)

    def step(slot, carry):
        @pl.when(slot > x)
        def _():
            whole_block(qT, kv, own, acc, best, slot)

        return carry

    lax.fori_loop(1, 4, step, 0)


def more_body(shifts, last, *refs):
    n = len(shifts)
    place, qT, bias = refs[:3]
    kvs = refs[3 : 3 + n]
    acc_in, best_in = refs[3 + n : 5 + n]
    z = place[2]
    if last:
        out, acc, best = refs[5 + n :]
        acc[...] = acc_in[...]
        best[...] = best_in[...]
    else:
        acc, best = refs[5 + n :]
        acc[...] = acc_in[...]
        best[...] = best_in[...]
    for shift, kv in zip(shifts, kvs):
        source = lax.rem(z - shift + 8, 8)

        @pl.when(source < z)
        def _(kv=kv, source=source):
            own = bias.at[source]

            def step(slot, carry):
                whole_block(qT, kv, own, acc, best, slot)
                return carry

            lax.fori_loop(0, 4, step, 0)

    if last:
        for slot in range(4):
            stats = []
            for h in range(2):
                total = acc[slot, h, 64:65, :]
                total = jnp.where(total > 0.0, total, 1.0)
                out[slot, h * HEAD : (h + 1) * HEAD, :] = (
                    acc[slot, h, :HEAD, :] / total
                ).astype(BF16)
                log_sum = best[slot, h] + jnp.log2(total)
                hi = log_sum.astype(BF16).astype(F32)
                mid = (log_sum - hi).astype(BF16).astype(F32)
                low = log_sum - hi - mid
                stats += [hi, mid, low]
            stats.append(jnp.zeros((10, 512), F32))
            out[slot, 128:144, :] = jnp.concatenate(stats, axis=0).astype(BF16)


STATE = (
    jax.ShapeDtypeStruct((4, 2, 80, 512), F32),
    jax.ShapeDtypeStruct((4, 2, 1, 512), F32),
)


def attend_first(place, qT, kv, bias):
    return pl.pallas_call(
        first_body,
        out_shape=STATE,
        in_specs=[sspec(), vspec(), vspec(), vspec()],
        out_specs=(vspec(), vspec()),
        name="attend_first",
    )(place, qT, kv, bias)


def attend_more(place, qT, bias, kvs, shifts, state, last):
    def body(*refs):
        more_body(shifts, last, *refs)

    if last:
        out_shape = jax.ShapeDtypeStruct((4, 144, 512), BF16)
        out_specs = vspec()
        scratch = [pltpu.VMEM(s.shape, s.dtype) for s in STATE]
    else:
        out_shape = STATE
        out_specs = (vspec(), vspec())
        scratch = []
    return pl.pallas_call(
        body,
        out_shape=out_shape,
        in_specs=[sspec()] + [vspec()] * (4 + len(kvs)),
        out_specs=out_specs,
        scratch_shapes=scratch,
        name="attend_last" if last else "attend_more",
    )(place, qT, bias, *kvs, *state)


def merge_body(own, r1, r2, r3, cum, rows_out, log_out):
    parts = (own, r1, r2, r3)
    for h in range(2):
        logs = []
        for part in parts:
            stats = part[128:144, :].astype(F32)
            logs.append(
                stats[3 * h : 3 * h + 1] + stats[3 * h + 1 : 3 * h + 2] + stats[3 * h + 2 : 3 * h + 3]
            )
        top = jnp.maximum(jnp.maximum(logs[0], logs[1]), jnp.maximum(logs[2], logs[3]))
        ws = [jnp.exp2(v - top) for v in logs]
        total = ws[0] + ws[1] + ws[2] + ws[3]
        o = jnp.zeros((HEAD, 512), F32)
        for part, w in zip(parts, ws):
            o = o + part[h * HEAD : (h + 1) * HEAD, :].astype(F32) * w
        rows_out[:, h * HEAD : (h + 1) * HEAD] = jnp.transpose(o / total).astype(BF16)
        log_out[h : h + 1, :] = (top + jnp.log2(total)) * LN2 + cum[h : h + 1, :]


def merge(own, others, cum):
    return pl.pallas_call(
        merge_body,
        out_shape=(
            jax.ShapeDtypeStruct((512, 128), BF16),
            jax.ShapeDtypeStruct((2, 512), F32),
        ),
        in_specs=[vspec()] * 5,
        out_specs=(vspec(), vspec()),
        name="merge",
    )(own, *others, cum)


def per_device(
    tokens,
    norm_gain,
    w_query,
    w_key,
    w_value,
    conv_in,
    conv_gate,
    conv_taps,
    conv_gain,
    cum_gate,
    out_attn,
    out_conv,
):
    z = lax.axis_index("z")
    x = lax.axis_index("x")
    y = lax.axis_index("y")
    c = lax.axis_index("c")
    place = jnp.stack([y, c, z, x]).astype(jnp.int32)

    wide = tokens.astype(F32)
    factor = lax.rsqrt(jnp.mean(wide * wide, axis=1, keepdims=True) + 1e-06)
    n0 = (wide * factor * norm_gain[None, :]).astype(BF16)
    n0 = lax.optimization_barrier(n0)
    own = [n0] + [turn(n0, "y", k) for k in (1, 2, 3)]
    partner = [turn(piece, "c", 1) for piece in own]

    cums = cum_gate.reshape(2, 8, 4, 512)
    column = lax.dynamic_index_in_dim(cums, x, 2, keepdims=False)
    base = lax.dynamic_slice(cum_gate, (0, z * 2048), (2, 1))
    rel = (base[:, :, None] - column) * LOG2E
    hi = lax.reduce_precision(rel, 8, 7)
    mid = lax.reduce_precision(rel - hi, 8, 7)
    low = rel - hi - mid
    split = jnp.stack([hi, mid, low], axis=1).reshape(6, 8, 512)
    bias = jnp.pad(jnp.transpose(split, (1, 2, 0)), ((0, 0), (0, 0), (0, 122))).astype(BF16)
    cum_own = lax.dynamic_slice(cum_gate, (0, (4 * z + x) * 512), (2, 512)) - base

    qT, kv, gated = project(
        place,
        own + partner,
        (w_query, w_key, w_value, conv_in, conv_gate),
    )

    a1 = turn(kv, "z", 1)
    b1 = turn(kv, "z", -1)
    qs = jnp.stack([qT] + [turn(qT, "x", k) for k in (1, 2, 3)])
    a2 = turn(a1, "z", 1)
    b2 = turn(b1, "z", -1)
    a3 = turn(a2, "z", 1)
    b3 = turn(b2, "z", -1)
    far = jnp.concatenate([turn(a3[:512], "z", 1), turn(b3[512:], "z", -1)], axis=0)

    state = attend_first(place, qs, kv, bias)
    state = attend_more(place, qs, bias, (a1, b1), (1, -1), state, False)
    state = attend_more(place, qs, bias, (a2, b2), (2, -2), state, False)
    outs = attend_more(place, qs, bias, (a3, b3, far), (3, -3, 4), state, True)
    others = [turn(outs[k], "x", -k) for k in (1, 2, 3)]
    rows, log_total = merge(outs[0], others, cum_own)

    rows_here = 512
    kernel_len = conv_taps.shape[0]
    pairs = [(i, i + 1) for i in range(31)]
    rim = lax.ppermute(gated[rows_here - 32 :], ("z", "x"), pairs)
    padded = jnp.concatenate([rim[2:], gated], axis=0).astype(F32)
    convolved = jnp.zeros((rows_here, 256), F32)
    for tap in range(kernel_len):
        convolved = convolved + conv_taps[tap][None, :] * padded[tap : tap + rows_here]
    square = jnp.sum(convolved * convolved, axis=1)
    square = square + turn(square, "c", 1)
    square = square + lax.ppermute(square, "y", [(i, i ^ 1) for i in range(4)])
    square = square + lax.ppermute(square, "y", [(i, i ^ 2) for i in range(4)])
    square = square / (256 * 8)
    conv_out = jax.nn.silu(
        convolved * lax.rsqrt(square + 1e-06)[:, None] * conv_gain[None, :]
    ).astype(BF16)
    part = jnp.dot(conv_out, out_conv, preferred_element_type=F32).reshape(4, 2, 64, 2048)
    mine = lax.dynamic_index_in_dim(part, c, 1, keepdims=False)
    theirs = lax.dynamic_index_in_dim(part, 1 - c, 1, keepdims=False).astype(BF16)
    both = (mine + turn(theirs, "c", 1).astype(F32)).astype(BF16)
    total = lax.dynamic_index_in_dim(both, y, 0, keepdims=False).astype(F32)
    for k in (1, 2, 3):
        piece = lax.dynamic_index_in_dim(both, lax.rem(y + k, 4), 0, keepdims=False)
        total = total + turn(piece, "y", k).astype(F32)

    wa = after(out_attn, kv)
    was = [wa] + [turn(wa, "y", k) for k in (1, 2, 3)]
    was = was + [turn(w, "c", 1) for w in was]

    by_owner = rows.reshape(4, 2, 64, 128)

    def for_owner(k, cc):
        return lax.dynamic_slice(by_owner, (lax.rem(y + k, 4), cc, 0, 0), (1, 1, 64, 128)).reshape(
            64, 128
        )

    heads = [for_owner(0, c)]
    heads += [turn(for_owner(k, c), "y", k) for k in (1, 2, 3)]
    heads += [turn_both(for_owner(k, 1 - c), k) for k in (0, 1, 2, 3)]
    mixed = total + jnp.dot(
        jnp.concatenate(heads, axis=1),
        jnp.concatenate(was, axis=0),
        preferred_element_type=F32,
    )
    return (mixed.astype(BF16), log_total)


def solution(mesh):
    grid = Mesh(mesh.devices.reshape(8, 4, 4, 2), ("z", "x", "y", "c"))
    sp = ("z", "x")
    tp = ("y", "c")
    in_specs = (
        P(sp + tp, None),
        P(),
        P(None, tp),
        P(None, tp),
        P(None, tp),
        P(None, tp),
        P(None, tp),
        P(None, tp),
        P(tp),
        P(tp, None),
        P(tp, None),
        P(tp, None),
    )
    out_specs = (P(sp + tp, None), P(tp, sp))
    return jax.shard_map(
        per_device, mesh=grid, in_specs=in_specs, out_specs=out_specs, check_vma=False
    )
```

```python
import math

import jax
import jax.numpy as jnp
from jax import lax
from jax.experimental import pallas as pl
from jax.experimental.pallas import tpu as pltpu
from jax.sharding import Mesh, PartitionSpec as P


HEAD = 64
LOG2E = math.log2(math.e)
LN2 = math.log(2.0)
NEG = -1e30
F32 = jnp.float32
BF16 = jnp.bfloat16
VMEM = pltpu.MemorySpace.VMEM
SMEM = pltpu.MemorySpace.SMEM
PARAMS = pltpu.CompilerParams(vmem_limit_bytes=24 * 2**20)


def vspec():
    return pl.BlockSpec(memory_space=VMEM)


def sspec():
    return pl.BlockSpec(memory_space=SMEM)


def turn(array, axis, by):
    n = lax.axis_size(axis)
    return lax.ppermute(array, axis, [(i, (i + by) % n) for i in range(n)])


def kernel(body, outs, args, scratch=(), aliases=None, scalars=1, far=False):
    spec = pl.BlockSpec(memory_space=pltpu.MemorySpace.HBM) if far else vspec()
    return pl.pallas_call(
        body,
        out_shape=outs,
        in_specs=[sspec()] * scalars + [spec] * (len(args) - scalars),
        out_specs=jax.tree.map(lambda _: vspec(), outs),
        scratch_shapes=list(scratch),
        input_output_aliases=aliases or {},
        compiler_params=PARAMS,
    )(*args)


def shape(*dims, dtype=BF16):
    return jax.ShapeDtypeStruct(dims, dtype)


def after(x, other):
    return lax.optimization_barrier((x, other))[0]


WIDTHS = (128, 128, 128, 256, 256)


def load_body(*refs):
    weights, out, sems = refs[:5], refs[5], refs[6]
    copies, at = [], 0
    for k, (ref, width) in enumerate(zip(weights, WIDTHS)):
        copies.append(pltpu.make_async_copy(ref, out.at[:, at : at + width], sems.at[k]))
        at += width
    for copy in copies:
        copy.start()
    for copy in copies:
        copy.wait()


def project_body(
    place, n0, n1, n2, n3, p0, p1, p2, p3, weights, q_out, kv_out, gated_out, rim_out, xs
):
    y = place[0]
    c = place[1]
    for k, (own, other) in enumerate(((n0, p0), (n1, p1), (n2, p2), (n3, p3))):
        at = lax.rem(y + 4 - k, 4) * 128
        xs[pl.ds(pl.multiple_of(at + c * 64, 64), 64), :] = own[...]
        xs[pl.ds(pl.multiple_of(at + (1 - c) * 64, 64), 64), :] = other[...]
    x = xs[...]
    qk = jnp.dot(x, weights[:, :256], preferred_element_type=F32)
    q_out[...] = jnp.transpose(qk[:, :128] * (LOG2E * HEAD**-0.5)).astype(BF16)
    kv_out[:512, :] = qk[:, 128:].astype(BF16)
    v = jnp.transpose(jnp.dot(x, weights[:, 256:384], preferred_element_type=F32)).astype(BF16)
    for j in range(4):
        kv_out[512 + 128 * j : 640 + 128 * j, :] = v[:, 128 * j : 128 * j + 128]
    opened = jnp.dot(x, weights[:, 384:640], preferred_element_type=F32)
    gating = jnp.dot(x, weights[:, 640:], preferred_element_type=F32)
    gated = (opened * jax.nn.sigmoid(gating)).astype(BF16)
    gated_out[...] = gated
    rim_out[...] = gated[480:]


def norm_body(tokens_far, gain_far, out, tokens, gain, sems):
    copies = [
        pltpu.make_async_copy(tokens_far, tokens, sems.at[0]),
        pltpu.make_async_copy(gain_far, gain, sems.at[1]),
    ]
    for copy in copies:
        copy.start()
    for copy in copies:
        copy.wait()
    wide = tokens[...].astype(F32)
    factor = lax.rsqrt(jnp.mean(wide * wide, axis=1, keepdims=True) + 1e-06)
    out[...] = (wide * factor * gain[...]).astype(BF16)


def bias_body(place, cum, bias, own):
    z = place[2]
    x = place[3]
    base = cum[:, pl.ds(pl.multiple_of(z * 2048, 128), 128)][:, :1]
    for b in range(8):
        at = pl.multiple_of((4 * b + x) * 512, 512)
        rel = (base - cum[:, pl.ds(at, 512)]) * LOG2E
        hi = rel.astype(BF16).astype(F32)
        mid = (rel - hi).astype(BF16).astype(F32)
        low = rel - hi - mid
        rows = [part[h : h + 1] for h in range(2) for part in (hi, mid, low)]
        rows = jnp.concatenate(rows + [jnp.zeros((122, 512), F32)], axis=0)
        bias[b] = jnp.transpose(rows).astype(BF16)
    at = pl.multiple_of((4 * z + x) * 512, 512)
    own[...] = cum[:, pl.ds(at, 512)] - base


def conv_body(gated, rim, taps, convolved, square, shifted):
    whole = jnp.concatenate([rim[...], gated[...]], axis=0).astype(F32)
    shifted[0] = whole
    for s in range(1, 8):
        shifted[s, :536] = whole[s : s + 536]

    def block(i, carry):
        at = pl.multiple_of(i * 128, 128)
        total = jnp.zeros((128, 256), F32)
        for tap in range(31):
            a, s = divmod(tap + 2, 8)
            total = total + taps[tap : tap + 1, :] * shifted[s, pl.ds(at + 8 * a, 128), :]
        convolved[pl.ds(at, 128), :] = total
        both = total * total
        both = jnp.transpose(both[:, :128] + both[:, 128:])
        square[:, pl.ds(at, 128)] = jnp.sum(both, axis=0, keepdims=True)
        return carry

    lax.fori_loop(0, 4, block, 0)


def gate_body(place, convolved, s0, s1, s2, s3, gain, weights, mine, theirs, left):
    c = place[1]
    square = (s0[...] + s1[...] + s2[...] + s3[...]) / 2048.0
    column = jnp.transpose(jnp.broadcast_to(lax.rsqrt(square + 1e-06), (128, 512)))
    factor = jnp.concatenate([column, column], axis=1)
    v = convolved[...] * factor * gain[...]
    left[...] = (v / (1.0 + jnp.exp(-v))).astype(BF16)

    def block(y, carry):
        rows = left[pl.ds(pl.multiple_of(128 * y, 128), 128), :]
        part = jnp.dot(rows, weights[...], preferred_element_type=F32).astype(BF16)

        @pl.when(c == 0)
        def _():
            mine[y] = part[:64]
            theirs[y] = part[64:]

        @pl.when(c == 1)
        def _():
            mine[y] = part[64:]
            theirs[y] = part[:64]

        return carry

    lax.fori_loop(0, 4, block, 0)


def fold_body(place, mine, theirs, own, f1, f2, f3):
    y = place[0]
    for k, ref in enumerate((own, f1, f2, f3)):
        at = lax.rem(y + k, 4)
        total = mine[at].astype(F32) + theirs[at].astype(F32)
        ref[...] = total.astype(ref.dtype)


def part_body(place, own, h0, h1, h2, h3, w0, w1, w2a, w2b, w3, mine, theirs):
    c = place[1]
    left = jnp.concatenate([h0[...], h1[...], h2[...], h3[...]], axis=1)
    right = jnp.concatenate([w0[...], w1[...], w2a[...], w2b[...], w3[...]], axis=0)
    both = jnp.dot(left, right, preferred_element_type=F32)

    @pl.when(c == 0)
    def _():
        mine[...] = both[:64] + own[...]
        theirs[...] = both[64:].astype(BF16)

    @pl.when(c == 1)
    def _():
        mine[...] = both[64:] + own[...]
        theirs[...] = both[:64].astype(BF16)


def final_body(mine, theirs, f1, f2, f3, out):
    folded = f1[...].astype(F32) + f2[...].astype(F32) + f3[...].astype(F32)
    out[...] = (mine[...] + theirs[...].astype(F32) + folded).astype(BF16)


DEPTH = 4


def tiles_of(slots):
    return [(s, h, lo) for s in range(slots) for h in range(2) for lo in (0, 256)]


def scores_tile(tile, at, q, kv, bias, slot, s_buf, top, offset):
    _, h, lo = tile
    block = q[slot, h * HEAD : (h + 1) * HEAD, lo : lo + 256]
    zero = jnp.zeros((HEAD, 256), BF16)
    row = lax.broadcasted_iota(jnp.int32, (128, 256), 0)
    pick = jnp.where((row >= 3 * h) & (row < 3 * h + 3), 1.0, 0.0).astype(BF16)
    rhs = jnp.concatenate([block, zero, pick] if h == 0 else [zero, block, pick], axis=0)
    lhs = jnp.concatenate([kv[:512, :], bias[...]], axis=1)
    s = jnp.dot(lhs, rhs, preferred_element_type=F32)
    if offset is not None:
        kk = lax.broadcasted_iota(jnp.int32, (512, 256), 0)
        qq = lax.broadcasted_iota(jnp.int32, (512, 256), 1) + (lo + offset)
        s = jnp.where(kk <= qq, s, NEG)
    s_buf[at % DEPTH] = s
    top[at % DEPTH] = jnp.max(s, axis=0, keepdims=True)


def weights_tile(tile, at, slot, best, s_buf, top, p_buf, shrink):
    _, h, lo = tile
    old = best[slot, h, :, lo : lo + 256]
    new = jnp.maximum(old, top[at % DEPTH])
    p_buf[at % DEPTH] = jnp.exp2(s_buf[at % DEPTH] - new).astype(BF16)
    best[slot, h, :, lo : lo + 256] = new
    shrink[at % DEPTH] = jnp.exp2(old - new)


def values_tile(tile, at, kv, slot, acc, p_buf, shrink):
    _, h, lo = tile
    vT = jnp.concatenate(
        [kv[512 + 128 * j + h * HEAD : 512 + 128 * j + (h + 1) * HEAD, :] for j in range(4)],
        axis=1,
    )
    vT = jnp.concatenate([vT, jnp.ones((16, 512), BF16)], axis=0)
    pv = jnp.dot(vT, p_buf[at % DEPTH], preferred_element_type=F32)
    acc[slot, h, :, lo : lo + 256] = (
        acc[slot, h, :, lo : lo + 256] * shrink[at % DEPTH] + pv
    )


def run_items(
    slots, count, block_of, bias_of, slot_of, offset_of, q, kvs, bias, acc, best, s_buf, top, p_buf, shrink
):
    tiles = tiles_of(slots)
    n = len(tiles)
    p_buf[(n - 1) % DEPTH] = jnp.zeros(p_buf.shape[1:], BF16)
    shrink[(n - 1) % DEPTH] = jnp.ones(shrink.shape[1:], F32)

    def scores(t, i):
        offset = None if offset_of is None else offset_of(i)
        slot = slot_of(i) + tiles[t][0]
        kv = kvs.at[block_of(i)]
        scores_tile(tiles[t], t, q, kv, bias.at[bias_of(i)], slot, s_buf, top, offset)

    def values(t, i):
        slot = slot_of(i) + tiles[t][0]
        values_tile(tiles[t], t, kvs.at[block_of(i)], slot, acc, p_buf, shrink)

    scores(0, 0)

    def step(i, carry):
        before = jnp.maximum(i - 1, 0)
        behind = jnp.minimum(i + 1, count - 1)
        for t in range(n):
            if t < n - 1:
                scores(t + 1, i)
            else:
                scores(0, behind)
            weights_tile(tiles[t], t, slot_of(i) + tiles[t][0], best, s_buf, top, p_buf, shrink)
            if t > 0:
                values(t - 1, i)
            else:
                values(n - 1, before)
        return carry

    lax.fori_loop(0, count, step, 0)
    values(n - 1, count - 1)


STATE = (
    jax.ShapeDtypeStruct((4, 2, 80, 512), F32),
    jax.ShapeDtypeStruct((4, 2, 1, 512), F32),
)


def attend_scratch(blocks):
    return [
        pltpu.VMEM((blocks, 1024, 128), BF16),
        pltpu.VMEM((DEPTH, 512, 256), F32),
        pltpu.VMEM((DEPTH, 1, 256), F32),
        pltpu.VMEM((DEPTH, 512, 256), BF16),
        pltpu.VMEM((DEPTH, 1, 256), F32),
    ]


def first_body(place, q0, q1, q2, q3, kv, bias, acc, best, q, kvs, s_buf, top, p_buf, shrink):
    z = place[2]
    x = place[3]
    for k, ref in enumerate((q0, q1, q2, q3)):
        q[k] = ref[...]
    kvs[0] = kv[...]
    acc[...] = jnp.zeros(acc.shape, F32)
    best[...] = jnp.full(best.shape, NEG, F32)
    run_items(
        1,
        4 - x,
        lambda i: 0,
        lambda i: z,
        lambda i: jnp.where(i == 0, 0, x + i),
        lambda i: jnp.where(i == 0, 0, 512),
        q, kvs, bias, acc, best, s_buf, top, p_buf, shrink,
    )


def more_body(shifts, last, place, q, bias, *refs):
    n = len(shifts)
    m = n + last
    blocks = refs[:m]
    if last:
        outs = refs[m + 2 : m + 6]
        acc, best, kvs, s_buf, top, p_buf, shrink = refs[m + 6 :]
    else:
        acc, best, kvs, s_buf, top, p_buf, shrink = refs[m + 2 :]
    z = place[2]
    count = 0
    for shift in shifts:
        count = count + jnp.where(z >= shift % 8, 2, 0)

    def source(b):
        shift = jnp.int32(shifts[-1])
        for k in range(n - 1):
            shift = jnp.where(b == k, shifts[k], shift)
        return lax.rem(z - shift + 8, 8)

    @pl.when(count > 0)
    def _():
        if last:
            kvs[0] = blocks[0][...]
            kvs[1, :512] = blocks[1][...]
            kvs[1, 512:] = blocks[2][...]
            kvs[2] = blocks[3][...]
        else:
            for k, ref in enumerate(blocks):
                kvs[k] = ref[...]

        def block(i):
            return i // 2 if isinstance(i, int) else lax.shift_right_logical(i, 1)

        run_items(
            2,
            count,
            block,
            lambda i: source(block(i)),
            lambda i: 2 * (i % 2) if isinstance(i, int) else 2 * lax.bitwise_and(i, 1),
            None,
            q, kvs, bias, acc, best, s_buf, top, p_buf, shrink,
        )

    if last:
        for slot in range(4):
            stats = []
            for h in range(2):
                total = acc[slot, h, 64:65, :]
                total = jnp.where(total > 0.0, total, 1.0)
                outs[slot][h * HEAD : (h + 1) * HEAD, :] = (
                    acc[slot, h, :HEAD, :] / total
                ).astype(BF16)
                log_sum = best[slot, h] + jnp.log2(total)
                hi = log_sum.astype(BF16).astype(F32)
                mid = (log_sum - hi).astype(BF16).astype(F32)
                low = log_sum - hi - mid
                stats += [hi, mid, low]
            stats.append(jnp.zeros((10, 512), F32))
            outs[slot][128:144, :] = jnp.concatenate(stats, axis=0).astype(BF16)


def attend_first(place, qs, kv, bias):
    return kernel(
        first_body, STATE + (shape(4, 128, 512),), (place, *qs, kv, bias), attend_scratch(1)
    )


def attend_more(place, q, bias, kvs, shifts, state, last=False):
    def body(*refs):
        more_body(shifts, last, *refs)

    if last:
        first, (upper, lower), third = kvs
        kvs = (first, upper, lower, third)
    n = len(kvs)
    outs = (shape(144, 512),) * 4 if last else ()
    aliases = {3 + n: len(outs), 4 + n: len(outs) + 1}
    scratch = attend_scratch(len(shifts))
    return kernel(body, outs + STATE, (place, q, bias, *kvs, *state), scratch, aliases)


def merge_body(place, own, r1, r2, r3, cum, log_out, *refs):
    pieces, rows = refs[:4], refs[4]
    y = place[0]
    parts = (own, r1, r2, r3)
    for h in range(2):
        logs = []
        for part in parts:
            stats = part[128:144, :].astype(F32)
            logs.append(
                stats[3 * h : 3 * h + 1] + stats[3 * h + 1 : 3 * h + 2] + stats[3 * h + 2 : 3 * h + 3]
            )
        peak = jnp.maximum(jnp.maximum(logs[0], logs[1]), jnp.maximum(logs[2], logs[3]))
        ws = [jnp.exp2(v - peak) for v in logs]
        total = ws[0] + ws[1] + ws[2] + ws[3]
        o = jnp.zeros((HEAD, 512), F32)
        for part, w in zip(parts, ws):
            o = o + part[h * HEAD : (h + 1) * HEAD, :].astype(F32) * w
        rows[:, h * HEAD : (h + 1) * HEAD] = jnp.transpose(o / total)
        log_out[h : h + 1, :] = (peak + jnp.log2(total)) * LN2 + cum[h : h + 1, :]
    for k in range(4):
        at = pl.multiple_of(lax.rem(y + k, 4) * 128, 128)
        pieces[k][...] = rows[pl.ds(at, 128), :].astype(BF16)


def per_device(
    tokens,
    norm_gain,
    w_query,
    w_key,
    w_value,
    conv_in,
    conv_gate,
    conv_taps,
    conv_gain,
    cum_gate,
    out_attn,
    out_conv,
):
    z = lax.axis_index("z")
    x = lax.axis_index("x")
    y = lax.axis_index("y")
    c = lax.axis_index("c")
    place = jnp.stack([y, c, z, x]).astype(jnp.int32)

    n0 = kernel(
        norm_body,
        shape(64, 2048),
        (tokens, norm_gain[None, :]),
        [
            pltpu.VMEM((64, 2048), BF16),
            pltpu.VMEM((1, 2048), F32),
            pltpu.SemaphoreType.DMA((2,)),
        ],
        scalars=0,
        far=True,
    )
    own = [n0] + [turn(n0, "y", k) for k in (1, 2, 3)]
    partner = [turn(piece, "c", 1) for piece in own]

    weights = kernel(
        load_body,
        shape(2048, 896),
        (w_query, w_key, w_value, conv_in, conv_gate),
        [pltpu.SemaphoreType.DMA((5,))],
        scalars=0,
        far=True,
    )
    bias, cum_own = kernel(
        bias_body, (shape(8, 512, 128), shape(2, 512, dtype=F32)), (place, cum_gate)
    )

    qT, kv, gated, rim = kernel(
        project_body,
        (shape(128, 512), shape(1024, 128), shape(512, 256), shape(32, 256)),
        (place, *own, *partner, weights),
        [pltpu.VMEM((512, 2048), BF16)],
    )

    rim = lax.ppermute(rim, ("z", "x"), [(i, i + 1) for i in range(31)])
    a1 = turn(kv, "z", 1)
    b1 = turn(kv, "z", -1)
    qs = [qT] + [turn(qT, "x", k) for k in (1, 2, 3)]
    a2 = turn(a1, "z", 1)
    b2 = turn(b1, "z", -1)
    a3 = turn(a2, "z", 1)
    b3 = turn(b2, "z", -1)
    fa = turn(a3[:512], "z", 1)
    fb = turn(b3[512:], "z", -1)

    convolved, square = kernel(
        conv_body,
        (shape(512, 256, dtype=F32), shape(1, 512, dtype=F32)),
        (gated, rim, conv_taps),
        [pltpu.VMEM((8, 544, 256), F32)],
        scalars=0,
    )
    square = square + turn(square, "c", 1)
    squares = [square] + [turn(square, "y", k) for k in (1, 2, 3)]
    mine, theirs = kernel(
        gate_body,
        (shape(4, 64, 2048), shape(4, 64, 2048)),
        (place, convolved, *squares, conv_gain[None, :], out_conv),
        [pltpu.VMEM((512, 256), BF16)],
    )
    theirs = turn(theirs, "c", 1)
    folded = kernel(
        fold_body, (shape(64, 2048, dtype=F32),) + (shape(64, 2048),) * 3, (place, mine, theirs)
    )
    folded = [folded[0]] + [turn(folded[k], "y", k) for k in (1, 2, 3)]

    w0 = after(out_attn, kv)
    w1 = turn(w0, "y", 1)
    w3 = turn(w0, "y", 3)
    w2a = turn(w1[:64], "y", 1)
    w2b = turn(w3[64:], "y", 3)

    *state, q = attend_first(place, qs, kv, bias)
    state = attend_more(place, q, bias, (a1, b1), (1, -1), state)
    state = attend_more(place, q, bias, (a2, b2), (2, -2), state)
    outs = attend_more(place, q, bias, (a3, (fa, fb), b3), (3, 4, -3), state, True)
    others = [turn(outs[k], "x", -k) for k in (1, 2, 3)]
    log_total, *pieces = kernel(
        merge_body,
        (shape(2, 512, dtype=F32),) + (shape(128, 128),) * 4,
        (place, outs[0], *others, cum_own),
        [pltpu.VMEM((512, 128), F32)],
    )
    heads = [pieces[0]] + [turn(pieces[k], "y", k) for k in (1, 2, 3)]
    mine, theirs = kernel(
        part_body,
        (shape(64, 2048, dtype=F32), shape(64, 2048)),
        (place, folded[0], *heads, w0, w1, w2a, w2b, w3),
    )
    theirs = turn(theirs, "c", 1)
    mixed = kernel(final_body, shape(64, 2048), (mine, theirs, *folded[1:]), scalars=0)
    return (mixed, log_total)


def solution(mesh):
    grid = Mesh(mesh.devices.reshape(8, 4, 4, 2), ("z", "x", "y", "c"))
    sp = ("z", "x")
    tp = ("y", "c")
    in_specs = (
        P(sp + tp, None),
        P(),
        P(None, tp),
        P(None, tp),
        P(None, tp),
        P(None, tp),
        P(None, tp),
        P(None, tp),
        P(tp),
        P(tp, None),
        P(tp, None),
        P(tp, None),
    )
    out_specs = (P(sp + tp, None), P(tp, sp))

    return jax.shard_map(
        per_device, mesh=grid, in_specs=in_specs, out_specs=out_specs, check_vma=False
    )
```

```python
import math

import jax
import jax.numpy as jnp
from jax import lax
from jax.experimental import pallas as pl
from jax.experimental.pallas import tpu as pltpu
from jax.sharding import Mesh, PartitionSpec as P


HEAD = 64
LOG2E = math.log2(math.e)
LN2 = math.log(2.0)
NEG = -1e30
F32 = jnp.float32
BF16 = jnp.bfloat16
VMEM = pltpu.MemorySpace.VMEM
SMEM = pltpu.MemorySpace.SMEM
PARAMS = pltpu.CompilerParams(vmem_limit_bytes=20 * 2**20)


def vspec():
    return pl.BlockSpec(memory_space=VMEM)


def sspec():
    return pl.BlockSpec(memory_space=SMEM)


def turn(array, axis, by):
    n = lax.axis_size(axis)
    return lax.ppermute(array, axis, [(i, (i + by) % n) for i in range(n)])


def swap(array, axis, bit):
    n = lax.axis_size(axis)
    return lax.ppermute(array, axis, [(i, i ^ bit) for i in range(n)])


def kernel(body, outs, args, scratch=(), aliases=None, scalars=1, far=0):
    hbm = pltpu.MemorySpace.HBM
    near = len(args) - far
    args = (*args[:near], *(pltpu.with_memory_space_constraint(a, hbm) for a in args[near:]))
    specs = [sspec()] * scalars + [vspec()] * (near - scalars)
    return pl.pallas_call(
        body,
        out_shape=outs,
        in_specs=specs + [pl.BlockSpec(memory_space=hbm)] * far,
        out_specs=jax.tree.map(lambda _: vspec(), outs),
        scratch_shapes=list(scratch),
        input_output_aliases=aliases or {},
        compiler_params=PARAMS,
    )(*args)


def shape(*dims, dtype=BF16):
    return jax.ShapeDtypeStruct(dims, dtype)


WIDTHS = (128, 128, 128, 256, 256)


def load_body(*refs):
    weights, out, sems = refs[1:6], refs[6], refs[7]
    copies, at = [], 0
    for k, (ref, width) in enumerate(zip(weights, WIDTHS)):
        copies.append(pltpu.make_async_copy(ref, out.at[:, at : at + width], sems.at[k]))
        at += width
    for copy in copies:
        copy.start()
    for copy in copies:
        copy.wait()


def project_body(
    place, n0, n1, n2, n3, p0, p1, p2, p3, weights, q_out, kv_out, gated_out, rim_out, xs
):
    y = place[0]
    c = place[1]
    for k, (own, other) in enumerate(((n0, p0), (n1, p1), (n2, p2), (n3, p3))):
        at = lax.rem(y + 4 - k, 4) * 128
        xs[pl.ds(pl.multiple_of(at + c * 64, 64), 64), :] = own[...]
        xs[pl.ds(pl.multiple_of(at + (1 - c) * 64, 64), 64), :] = other[...]
    x = xs[...]
    qk = jnp.dot(x, weights[:, :256], preferred_element_type=F32)
    q_out[...] = jnp.transpose(qk[:, :128] * (LOG2E * HEAD**-0.5)).astype(BF16)
    kv_out[:512, :] = qk[:, 128:].astype(BF16)
    v = jnp.transpose(jnp.dot(x, weights[:, 256:384], preferred_element_type=F32)).astype(BF16)
    for j in range(4):
        kv_out[512 + 128 * j : 640 + 128 * j, :] = v[:, 128 * j : 128 * j + 128]
    opened = jnp.dot(x, weights[:, 384:640], preferred_element_type=F32)
    gating = jnp.dot(x, weights[:, 640:], preferred_element_type=F32)
    gated = (opened * jax.nn.sigmoid(gating)).astype(BF16)
    gated_out[...] = gated
    rim_out[...] = gated[480:]


def norm_body(tokens_far, gain_far, out, tokens, gain, sems):
    copies = [
        pltpu.make_async_copy(tokens_far, tokens, sems.at[0]),
        pltpu.make_async_copy(gain_far, gain, sems.at[1]),
    ]
    for copy in copies:
        copy.start()
    for copy in copies:
        copy.wait()
    wide = tokens[...].astype(F32)
    factor = lax.rsqrt(jnp.mean(wide * wide, axis=1, keepdims=True) + 1e-06)
    out[...] = (wide * factor * gain[...]).astype(BF16)


def bias_body(place, cum, bias, own):
    z = place[2]
    x = place[3]
    base = cum[:, pl.ds(pl.multiple_of(z * 2048, 128), 128)][:, :1]
    for b in range(8):
        at = pl.multiple_of((4 * b + x) * 512, 512)
        rel = (base - cum[:, pl.ds(at, 512)]) * LOG2E
        hi = rel.astype(BF16).astype(F32)
        mid = (rel - hi).astype(BF16).astype(F32)
        low = rel - hi - mid
        rows = [part[h : h + 1] for h in range(2) for part in (hi, mid, low)]
        rows = jnp.concatenate(rows + [jnp.zeros((122, 512), F32)], axis=0)
        bias[b] = jnp.transpose(rows).astype(BF16)
    at = pl.multiple_of((4 * z + x) * 512, 512)
    own[...] = cum[:, pl.ds(at, 512)] - base


def conv_body(gated, rim, taps, convolved, square, shifted):
    whole = jnp.concatenate([rim[...], gated[...]], axis=0).astype(F32)
    shifted[0] = whole
    for s in range(1, 8):
        shifted[s, :536] = whole[s : s + 536]

    def block(i, carry):
        at = pl.multiple_of(i * 128, 128)
        total = jnp.zeros((128, 256), F32)
        for tap in range(31):
            a, s = divmod(tap + 2, 8)
            total = total + taps[tap : tap + 1, :] * shifted[s, pl.ds(at + 8 * a, 128), :]
        convolved[pl.ds(at, 128), :] = total
        both = total * total
        both = jnp.transpose(both[:, :128] + both[:, 128:])
        square[:, pl.ds(at, 128)] = jnp.sum(both, axis=0, keepdims=True)
        return carry

    lax.fori_loop(0, 4, block, 0)


def gate_body(place, convolved, total, gain, weights, g0, g1, g2, g3, left):
    y = place[0]
    square = total[...] / 2048.0
    column = jnp.transpose(jnp.broadcast_to(lax.rsqrt(square + 1e-06), (128, 512)))
    factor = jnp.concatenate([column, column], axis=1)
    v = convolved[...] * factor * gain[...]
    left[...] = (v / (1.0 + jnp.exp(-v))).astype(BF16)
    for k, out in enumerate((g0, g1, g2, g3)):
        at = pl.multiple_of(lax.rem(y + k, 4) * 128, 128)
        rows = left[pl.ds(at, 128), :]
        out[...] = jnp.dot(rows, weights[...], preferred_element_type=F32).astype(BF16)


def part_body(place, h0, h1, h2, h3, g0, g1, g2, g3, w0, w1, w2, w3, mine, theirs, both):
    c = place[1]
    left = jnp.concatenate([h0[...], h1[...], h2[...], h3[...]], axis=1)
    right = jnp.concatenate([w0[...], w1[...], w2[...], w3[...]], axis=0)
    conv = g0[...].astype(F32) + g1[...].astype(F32) + g2[...].astype(F32) + g3[...].astype(F32)
    both[...] = jnp.dot(left, right, preferred_element_type=F32) + conv
    mine[...] = both[pl.ds(pl.multiple_of(c * 64, 64), 64), :]
    theirs[...] = both[pl.ds(pl.multiple_of((1 - c) * 64, 64), 64), :].astype(BF16)


def final_body(mine, theirs, out):
    out[...] = (mine[...] + theirs[...].astype(F32)).astype(BF16)


DEPTH = 4


def tiles_of(slots):
    return [(s, h, lo) for s in range(slots) for h in range(2) for lo in (0, 256)]


def scores_tile(tile, at, q, kv, bias, slot, s_buf, top, offset):
    _, h, lo = tile
    block = q[slot, h * HEAD : (h + 1) * HEAD, lo : lo + 256]
    zero = jnp.zeros((HEAD, 256), BF16)
    row = lax.broadcasted_iota(jnp.int32, (128, 256), 0)
    pick = jnp.where((row >= 3 * h) & (row < 3 * h + 3), 1.0, 0.0).astype(BF16)
    rhs = jnp.concatenate([block, zero, pick] if h == 0 else [zero, block, pick], axis=0)
    lhs = jnp.concatenate([kv[:512, :], bias[...]], axis=1)
    s = jnp.dot(lhs, rhs, preferred_element_type=F32)
    if offset is not None:
        kk = lax.broadcasted_iota(jnp.int32, (512, 256), 0)
        qq = lax.broadcasted_iota(jnp.int32, (512, 256), 1) + (lo + offset)
        s = jnp.where(kk <= qq, s, NEG)
    s_buf[at % DEPTH] = s
    top[at % DEPTH] = jnp.max(s, axis=0, keepdims=True)


def weights_tile(tile, at, slot, best, s_buf, top, p_buf, shrink):
    _, h, lo = tile
    old = best[slot, h, :, lo : lo + 256]
    new = jnp.maximum(old, top[at % DEPTH])
    p_buf[at % DEPTH] = jnp.exp2(s_buf[at % DEPTH] - new).astype(BF16)
    best[slot, h, :, lo : lo + 256] = new
    shrink[at % DEPTH] = jnp.exp2(old - new)


def values_tile(tile, at, kv, slot, acc, p_buf, shrink):
    _, h, lo = tile
    vT = jnp.concatenate(
        [kv[512 + 128 * j + h * HEAD : 512 + 128 * j + (h + 1) * HEAD, :] for j in range(4)],
        axis=1,
    )
    vT = jnp.concatenate([vT, jnp.ones((16, 512), BF16)], axis=0)
    pv = jnp.dot(vT, p_buf[at % DEPTH], preferred_element_type=F32)
    acc[slot, h, :, lo : lo + 256] = (
        acc[slot, h, :, lo : lo + 256] * shrink[at % DEPTH] + pv
    )


def run_items(
    slots, count, block_of, bias_of, slot_of, offset_of, q, kvs, bias, acc, best, s_buf, top, p_buf, shrink
):
    tiles = tiles_of(slots)
    n = len(tiles)
    p_buf[(n - 1) % DEPTH] = jnp.zeros(p_buf.shape[1:], BF16)
    shrink[(n - 1) % DEPTH] = jnp.ones(shrink.shape[1:], F32)

    def scores(t, i):
        offset = None if offset_of is None else offset_of(i)
        slot = slot_of(i) + tiles[t][0]
        kv = kvs.at[block_of(i)]
        scores_tile(tiles[t], t, q, kv, bias.at[bias_of(i)], slot, s_buf, top, offset)

    def values(t, i):
        slot = slot_of(i) + tiles[t][0]
        values_tile(tiles[t], t, kvs.at[block_of(i)], slot, acc, p_buf, shrink)

    scores(0, 0)

    def step(i, carry):
        before = jnp.maximum(i - 1, 0)
        behind = jnp.minimum(i + 1, count - 1)
        for t in range(n):
            if t < n - 1:
                scores(t + 1, i)
            else:
                scores(0, behind)
            weights_tile(tiles[t], t, slot_of(i) + tiles[t][0], best, s_buf, top, p_buf, shrink)
            if t > 0:
                values(t - 1, i)
            else:
                values(n - 1, before)
        return carry

    lax.fori_loop(0, count, step, 0)
    values(n - 1, count - 1)


STATE = (
    jax.ShapeDtypeStruct((4, 2, 80, 512), F32),
    jax.ShapeDtypeStruct((4, 2, 1, 512), F32),
)


def attend_scratch(blocks):
    return [
        pltpu.VMEM((blocks, 1024, 128), BF16),
        pltpu.VMEM((DEPTH, 512, 256), F32),
        pltpu.VMEM((DEPTH, 1, 256), F32),
        pltpu.VMEM((DEPTH, 512, 256), BF16),
        pltpu.VMEM((DEPTH, 1, 256), F32),
    ]


def first_body(place, q0, q1, q2, q3, kv, bias, acc, best, q, kvs, s_buf, top, p_buf, shrink):
    z = place[2]
    x = place[3]
    for k, ref in enumerate((q0, q1, q2, q3)):
        q[k] = ref[...]
    kvs[0] = kv[...]
    acc[...] = jnp.zeros(acc.shape, F32)
    best[...] = jnp.full(best.shape, NEG, F32)
    run_items(
        1,
        4 - x,
        lambda i: 0,
        lambda i: z,
        lambda i: jnp.where(i == 0, 0, x + i),
        lambda i: jnp.where(i == 0, 0, 512),
        q, kvs, bias, acc, best, s_buf, top, p_buf, shrink,
    )


def more_body(shifts, last, place, q, bias, *refs):
    n = len(shifts)
    m = n
    blocks = refs[:m]
    if last:
        outs = refs[m + 2 : m + 6]
        acc, best, kvs, s_buf, top, p_buf, shrink = refs[m + 6 :]
    else:
        acc, best, kvs, s_buf, top, p_buf, shrink = refs[m + 2 :]
    z = place[2]
    count = 0
    for shift in shifts:
        count = count + jnp.where(z >= shift % 8, 2, 0)

    def source(b):
        shift = jnp.int32(shifts[-1])
        for k in range(n - 1):
            shift = jnp.where(b == k, shifts[k], shift)
        return lax.rem(z - shift + 8, 8)

    @pl.when(count > 0)
    def _():
        for k, ref in enumerate(blocks):
            kvs[k] = ref[...]

        def block(i):
            return i // 2 if isinstance(i, int) else lax.shift_right_logical(i, 1)

        run_items(
            2,
            count,
            block,
            lambda i: source(block(i)),
            lambda i: 2 * (i % 2) if isinstance(i, int) else 2 * lax.bitwise_and(i, 1),
            None,
            q, kvs, bias, acc, best, s_buf, top, p_buf, shrink,
        )

    if last:
        for slot in range(4):
            stats = []
            for h in range(2):
                total = acc[slot, h, 64:65, :]
                total = jnp.where(total > 0.0, total, 1.0)
                outs[slot][h * HEAD : (h + 1) * HEAD, :] = (
                    acc[slot, h, :HEAD, :] / total
                ).astype(BF16)
                log_sum = best[slot, h] + jnp.log2(total)
                hi = log_sum.astype(BF16).astype(F32)
                mid = (log_sum - hi).astype(BF16).astype(F32)
                low = log_sum - hi - mid
                stats += [hi, mid, low]
            stats.append(jnp.zeros((10, 512), F32))
            outs[slot][128:144, :] = jnp.concatenate(stats, axis=0).astype(BF16)


def attend_first(place, qs, kv, bias):
    return kernel(
        first_body, STATE + (shape(4, 128, 512),), (place, *qs, kv, bias), attend_scratch(1)
    )


def attend_more(place, q, bias, kvs, shifts, state, last=False):
    def body(*refs):
        more_body(shifts, last, *refs)

    n = len(kvs)
    outs = (shape(144, 512),) * 4 if last else ()
    aliases = {3 + n: len(outs), 4 + n: len(outs) + 1}
    scratch = attend_scratch(len(shifts))
    return kernel(body, outs + STATE, (place, q, bias, *kvs, *state), scratch, aliases)


def merge_body(place, own, r1, r2, r3, cum, log_out, *refs):
    pieces, rows = refs[:4], refs[4]
    y = place[0]
    parts = (own, r1, r2, r3)
    for h in range(2):
        logs = []
        for part in parts:
            stats = part[128:144, :].astype(F32)
            logs.append(
                stats[3 * h : 3 * h + 1] + stats[3 * h + 1 : 3 * h + 2] + stats[3 * h + 2 : 3 * h + 3]
            )
        peak = jnp.maximum(jnp.maximum(logs[0], logs[1]), jnp.maximum(logs[2], logs[3]))
        ws = [jnp.exp2(v - peak) for v in logs]
        total = ws[0] + ws[1] + ws[2] + ws[3]
        o = jnp.zeros((HEAD, 512), F32)
        for part, w in zip(parts, ws):
            o = o + part[h * HEAD : (h + 1) * HEAD, :].astype(F32) * w
        rows[:, h * HEAD : (h + 1) * HEAD] = jnp.transpose(o / total)
        log_out[h : h + 1, :] = (peak + jnp.log2(total)) * LN2 + cum[h : h + 1, :]
    for k in range(4):
        at = pl.multiple_of(lax.rem(y + k, 4) * 128, 128)
        pieces[k][...] = rows[pl.ds(at, 128), :].astype(BF16)


def per_device(
    tokens,
    norm_gain,
    w_query,
    w_key,
    w_value,
    conv_in,
    conv_gate,
    conv_taps,
    conv_gain,
    cum_gate,
    out_attn,
    out_conv,
):
    z = lax.axis_index("z")
    x = lax.axis_index("x")
    y = lax.axis_index("y")
    c = lax.axis_index("c")
    place = jnp.stack([y, c, z, x]).astype(jnp.int32)

    n0 = kernel(
        norm_body,
        shape(64, 2048),
        (tokens, norm_gain[None, :]),
        [
            pltpu.VMEM((64, 2048), BF16),
            pltpu.VMEM((1, 2048), F32),
            pltpu.SemaphoreType.DMA((2,)),
        ],
        scalars=0,
        far=2,
    )
    own = [n0] + [turn(n0, "y", k) for k in (1, 2, 3)]
    partner = [turn(piece, "c", 1) for piece in own]

    ws = [out_attn] + [turn(out_attn, "y", k) for k in (1, 2, 3)]

    bias, cum_own = kernel(
        bias_body, (shape(8, 512, 128), shape(2, 512, dtype=F32)), (place, cum_gate)
    )
    weights = kernel(
        load_body,
        shape(2048, 896),
        (cum_own, w_query, w_key, w_value, conv_in, conv_gate),
        [pltpu.SemaphoreType.DMA((5,))],
        scalars=0,
        far=5,
    )

    qT, kv, gated, rim = kernel(
        project_body,
        (shape(128, 512), shape(1024, 128), shape(512, 256), shape(32, 256)),
        (place, *own, *partner, weights),
        [pltpu.VMEM((512, 2048), BF16)],
    )

    rim = lax.ppermute(rim, ("z", "x"), [(i, i + 1) for i in range(31)])
    a1 = turn(kv, "z", 1)
    b1 = turn(kv, "z", -1)
    qs = [qT] + [turn(qT, "x", k) for k in (1, 2, 3)]
    a2 = turn(a1, "z", 1)
    b2 = turn(b1, "z", -1)
    a3 = turn(a2, "z", 1)
    b3 = turn(b2, "z", -1)
    a4 = turn(a3, "z", 1)

    convolved, square = kernel(
        conv_body,
        (shape(512, 256, dtype=F32), shape(1, 512, dtype=F32)),
        (gated, rim, conv_taps),
        [pltpu.VMEM((8, 544, 256), F32)],
        scalars=0,
    )
    square = square + turn(square, "c", 1)
    square = square + swap(square, "y", 1)
    square = square + swap(square, "y", 2)
    parts = kernel(
        gate_body,
        (shape(128, 2048),) * 4,
        (place, convolved, square, conv_gain[None, :], out_conv),
        [pltpu.VMEM((512, 256), BF16)],
    )
    parts = [parts[0]] + [turn(parts[k], "y", k) for k in (1, 2, 3)]

    *state, q = attend_first(place, qs, kv, bias)
    state = attend_more(place, q, bias, (a1, b1), (1, -1), state)
    state = attend_more(place, q, bias, (a2, b2), (2, -2), state)
    outs = attend_more(place, q, bias, (a3, a4, b3), (3, 4, -3), state, True)
    others = [turn(outs[k], "x", -k) for k in (1, 2, 3)]
    log_total, *pieces = kernel(
        merge_body,
        (shape(2, 512, dtype=F32),) + (shape(128, 128),) * 4,
        (place, outs[0], *others, cum_own),
        [pltpu.VMEM((512, 128), F32)],
    )
    heads = [pieces[0]] + [turn(pieces[k], "y", k) for k in (1, 2, 3)]
    mine, theirs = kernel(
        part_body,
        (shape(64, 2048, dtype=F32), shape(64, 2048)),
        (place, *heads, *parts, *ws),
        [pltpu.VMEM((128, 2048), F32)],
    )
    theirs = turn(theirs, "c", 1)
    mixed = kernel(final_body, shape(64, 2048), (mine, theirs), scalars=0)
    return (mixed, log_total)


def solution(mesh):
    grid = Mesh(mesh.devices.reshape(8, 4, 4, 2), ("z", "x", "y", "c"))
    sp = ("z", "x")
    tp = ("y", "c")
    in_specs = (
        P(sp + tp, None),
        P(),
        P(None, tp),
        P(None, tp),
        P(None, tp),
        P(None, tp),
        P(None, tp),
        P(None, tp),
        P(tp),
        P(tp, None),
        P(tp, None),
        P(tp, None),
    )
    out_specs = (P(sp + tp, None), P(tp, sp))

    return jax.shard_map(
        per_device, mesh=grid, in_specs=in_specs, out_specs=out_specs, check_vma=False
    )
```

```python
import math

import jax
import jax.numpy as jnp
from jax import lax
from jax.experimental import pallas as pl
from jax.experimental.pallas import tpu as pltpu
from jax.sharding import Mesh, PartitionSpec as P


HEAD = 64
LOG2E = math.log2(math.e)
LN2 = math.log(2.0)
NEG = -1e30
F32 = jnp.float32
BF16 = jnp.bfloat16
VMEM = pltpu.MemorySpace.VMEM
SMEM = pltpu.MemorySpace.SMEM
PARAMS = pltpu.CompilerParams(vmem_limit_bytes=20 * 2**20)


def vspec():
    return pl.BlockSpec(memory_space=VMEM)


def sspec():
    return pl.BlockSpec(memory_space=SMEM)


def turn(array, axis, by):
    n = lax.axis_size(axis)
    return lax.ppermute(array, axis, [(i, (i + by) % n) for i in range(n)])


def swap(array, axis, bit):
    n = lax.axis_size(axis)
    return lax.ppermute(array, axis, [(i, i ^ bit) for i in range(n)])


def kernel(body, outs, args, scratch=(), aliases=None, scalars=1, far=0):
    hbm = pltpu.MemorySpace.HBM
    near = len(args) - far
    args = (*args[:near], *(pltpu.with_memory_space_constraint(a, hbm) for a in args[near:]))
    specs = [sspec()] * scalars + [vspec()] * (near - scalars)
    return pl.pallas_call(
        body,
        out_shape=outs,
        in_specs=specs + [pl.BlockSpec(memory_space=hbm)] * far,
        out_specs=jax.tree.map(lambda _: vspec(), outs),
        scratch_shapes=list(scratch),
        input_output_aliases=aliases or {},
        compiler_params=PARAMS,
    )(*args)


def shape(*dims, dtype=BF16):
    return jax.ShapeDtypeStruct(dims, dtype)


WIDTHS = (128, 128, 128, 256, 256)


def load_body(*refs):
    weights, out, sems = refs[1:6], refs[6], refs[7]
    copies, at = [], 0
    for k, (ref, width) in enumerate(zip(weights, WIDTHS)):
        copies.append(pltpu.make_async_copy(ref, out.at[:, at : at + width], sems.at[k]))
        at += width
    for copy in copies:
        copy.start()
    for copy in copies:
        copy.wait()


def project_body(
    place, n0, n1, n2, n3, p0, p1, p2, p3, weights, q_out, kv_out, gated_out, rim_out, xs
):
    y = place[0]
    c = place[1]
    for k, (own, other) in enumerate(((n0, p0), (n1, p1), (n2, p2), (n3, p3))):
        at = lax.rem(y + 4 - k, 4) * 128
        xs[pl.ds(pl.multiple_of(at + c * 64, 64), 64), :] = own[...]
        xs[pl.ds(pl.multiple_of(at + (1 - c) * 64, 64), 64), :] = other[...]
    x = xs[...]
    qk = jnp.dot(x, weights[:, :256], preferred_element_type=F32)
    q_out[...] = jnp.transpose(qk[:, :128] * (LOG2E * HEAD**-0.5)).astype(BF16)
    kv_out[:512, :] = qk[:, 128:].astype(BF16)
    v = jnp.transpose(jnp.dot(x, weights[:, 256:384], preferred_element_type=F32)).astype(BF16)
    for j in range(4):
        kv_out[512 + 128 * j : 640 + 128 * j, :] = v[:, 128 * j : 128 * j + 128]
    opened = jnp.dot(x, weights[:, 384:640], preferred_element_type=F32)
    gating = jnp.dot(x, weights[:, 640:], preferred_element_type=F32)
    gated = (opened * jax.nn.sigmoid(gating)).astype(BF16)
    gated_out[...] = gated
    rim_out[...] = gated[480:]


def norm_body(tokens_far, gain_far, out, tokens, gain, sems):
    copies = [
        pltpu.make_async_copy(tokens_far, tokens, sems.at[0]),
        pltpu.make_async_copy(gain_far, gain, sems.at[1]),
    ]
    for copy in copies:
        copy.start()
    for copy in copies:
        copy.wait()
    wide = tokens[...].astype(F32)
    factor = lax.rsqrt(jnp.mean(wide * wide, axis=1, keepdims=True) + 1e-06)
    out[...] = (wide * factor * gain[...]).astype(BF16)


def bias_body(place, cum, bias, own):
    z = place[2]
    x = place[3]
    base = cum[:, pl.ds(pl.multiple_of(z * 2048, 128), 128)][:, :1]
    for b in range(8):
        at = pl.multiple_of((4 * b + x) * 512, 512)
        rel = (base - cum[:, pl.ds(at, 512)]) * LOG2E
        hi = rel.astype(BF16).astype(F32)
        mid = (rel - hi).astype(BF16).astype(F32)
        low = rel - hi - mid
        rows = [part[h : h + 1] for h in range(2) for part in (hi, mid, low)]
        rows = jnp.concatenate(rows + [jnp.zeros((122, 512), F32)], axis=0)
        bias[b] = jnp.transpose(rows).astype(BF16)
    at = pl.multiple_of((4 * z + x) * 512, 512)
    own[...] = cum[:, pl.ds(at, 512)] - base


def conv_body(gated, rim, taps, convolved, square, shifted):
    whole = jnp.concatenate([rim[...], gated[...]], axis=0).astype(F32)
    shifted[0] = whole
    for s in range(1, 8):
        shifted[s, :536] = whole[s : s + 536]

    def block(i, carry):
        at = pl.multiple_of(i * 128, 128)
        total = jnp.zeros((128, 256), F32)
        for tap in range(31):
            a, s = divmod(tap + 2, 8)
            total = total + taps[tap : tap + 1, :] * shifted[s, pl.ds(at + 8 * a, 128), :]
        convolved[pl.ds(at, 128), :] = total
        both = total * total
        both = jnp.transpose(both[:, :128] + both[:, 128:])
        square[:, pl.ds(at, 128)] = jnp.sum(both, axis=0, keepdims=True)
        return carry

    lax.fori_loop(0, 4, block, 0)


def gate_body(place, convolved, total, gain, weights, g0, g1, g2, g3, left):
    y = place[0]
    square = total[...] / 2048.0
    column = jnp.transpose(jnp.broadcast_to(lax.rsqrt(square + 1e-06), (128, 512)))
    factor = jnp.concatenate([column, column], axis=1)
    v = convolved[...] * factor * gain[...]
    left[...] = (v / (1.0 + jnp.exp(-v))).astype(BF16)
    for k, out in enumerate((g0, g1, g2, g3)):
        at = pl.multiple_of(lax.rem(y + k, 4) * 128, 128)
        rows = left[pl.ds(at, 128), :]
        out[...] = jnp.dot(rows, weights[...], preferred_element_type=F32).astype(BF16)


def part_body(place, h0, h1, h2, h3, g0, g1, g2, g3, w0, w1, w2, w3, mine, theirs, both):
    c = place[1]
    left = jnp.concatenate([h0[...], h1[...], h2[...], h3[...]], axis=1)
    right = jnp.concatenate([w0[...], w1[...], w2[...], w3[...]], axis=0)
    conv = g0[...].astype(F32) + g1[...].astype(F32) + g2[...].astype(F32) + g3[...].astype(F32)
    both[...] = jnp.dot(left, right, preferred_element_type=F32) + conv
    mine[...] = both[pl.ds(pl.multiple_of(c * 64, 64), 64), :]
    theirs[...] = both[pl.ds(pl.multiple_of((1 - c) * 64, 64), 64), :].astype(BF16)


def final_body(mine, theirs, out):
    out[...] = (mine[...] + theirs[...].astype(F32)).astype(BF16)


DEPTH = 4


def tiles_of(slots):
    return [(s, h, lo) for s in range(slots) for h in range(2) for lo in (0, 256)]


def scores_tile(tile, at, q, kv, bias, slot, s_buf, top, offset):
    _, h, lo = tile
    block = q[slot, h * HEAD : (h + 1) * HEAD, lo : lo + 256]
    zero = jnp.zeros((HEAD, 256), BF16)
    row = lax.broadcasted_iota(jnp.int32, (128, 256), 0)
    pick = jnp.where((row >= 3 * h) & (row < 3 * h + 3), 1.0, 0.0).astype(BF16)
    rhs = jnp.concatenate([block, zero, pick] if h == 0 else [zero, block, pick], axis=0)
    lhs = jnp.concatenate([kv[:512, :], bias[...]], axis=1)
    s = jnp.dot(lhs, rhs, preferred_element_type=F32)
    if offset is not None:
        kk = lax.broadcasted_iota(jnp.int32, (512, 256), 0)
        qq = lax.broadcasted_iota(jnp.int32, (512, 256), 1) + (lo + offset)
        s = jnp.where(kk <= qq, s, NEG)
    s_buf[at % DEPTH] = s
    top[at % DEPTH] = jnp.max(s, axis=0, keepdims=True)


def weights_tile(tile, at, slot, best, s_buf, top, p_buf, shrink):
    _, h, lo = tile
    old = best[slot, h, :, lo : lo + 256]
    new = jnp.maximum(old, top[at % DEPTH])
    p_buf[at % DEPTH] = jnp.exp2(s_buf[at % DEPTH] - new).astype(BF16)
    best[slot, h, :, lo : lo + 256] = new
    shrink[at % DEPTH] = jnp.exp2(old - new)


def values_tile(tile, at, kv, slot, acc, p_buf, shrink):
    _, h, lo = tile
    vT = jnp.concatenate(
        [kv[512 + 128 * j + h * HEAD : 512 + 128 * j + (h + 1) * HEAD, :] for j in range(4)],
        axis=1,
    )
    vT = jnp.concatenate([vT, jnp.ones((16, 512), BF16)], axis=0)
    pv = jnp.dot(vT, p_buf[at % DEPTH], preferred_element_type=F32)
    acc[slot, h, :, lo : lo + 256] = (
        acc[slot, h, :, lo : lo + 256] * shrink[at % DEPTH] + pv
    )


def run_items(
    slots, count, block_of, bias_of, slot_of, offset_of, q, kvs, bias, acc, best, s_buf, top, p_buf, shrink
):
    tiles = tiles_of(slots)
    n = len(tiles)
    p_buf[(n - 1) % DEPTH] = jnp.zeros(p_buf.shape[1:], BF16)
    shrink[(n - 1) % DEPTH] = jnp.ones(shrink.shape[1:], F32)

    def scores(t, i):
        offset = None if offset_of is None else offset_of(i)
        slot = slot_of(i) + tiles[t][0]
        kv = kvs.at[block_of(i)]
        scores_tile(tiles[t], t, q, kv, bias.at[bias_of(i)], slot, s_buf, top, offset)

    def values(t, i):
        slot = slot_of(i) + tiles[t][0]
        values_tile(tiles[t], t, kvs.at[block_of(i)], slot, acc, p_buf, shrink)

    scores(0, 0)

    def step(i, carry):
        before = jnp.maximum(i - 1, 0)
        behind = jnp.minimum(i + 1, count - 1)
        for t in range(n):
            if t < n - 1:
                scores(t + 1, i)
            else:
                scores(0, behind)
            weights_tile(tiles[t], t, slot_of(i) + tiles[t][0], best, s_buf, top, p_buf, shrink)
            if t > 0:
                values(t - 1, i)
            else:
                values(n - 1, before)
        return carry

    lax.fori_loop(0, count, step, 0)
    values(n - 1, count - 1)


STATE = (
    jax.ShapeDtypeStruct((4, 2, 80, 512), F32),
    jax.ShapeDtypeStruct((4, 2, 1, 512), F32),
)


def attend_scratch(blocks):
    return [
        pltpu.VMEM((blocks, 1024, 128), BF16),
        pltpu.VMEM((DEPTH, 512, 256), F32),
        pltpu.VMEM((DEPTH, 1, 256), F32),
        pltpu.VMEM((DEPTH, 512, 256), BF16),
        pltpu.VMEM((DEPTH, 1, 256), F32),
    ]


def first_body(place, q0, q1, q2, q3, kv, bias, acc, best, q, kvs, s_buf, top, p_buf, shrink):
    z = place[2]
    x = place[3]
    for k, ref in enumerate((q0, q1, q2, q3)):
        q[k] = ref[...]
    kvs[0] = kv[...]
    acc[...] = jnp.zeros(acc.shape, F32)
    best[...] = jnp.full(best.shape, NEG, F32)
    run_items(
        1,
        4 - x,
        lambda i: 0,
        lambda i: z,
        lambda i: jnp.where(i == 0, 0, x + i),
        lambda i: jnp.where(i == 0, 0, 512),
        q, kvs, bias, acc, best, s_buf, top, p_buf, shrink,
    )


def more_body(shifts, last, place, q, bias, *refs):
    n = len(shifts)
    m = n
    blocks = refs[:m]
    if last:
        outs = refs[m + 2 : m + 6]
        acc, best, kvs, s_buf, top, p_buf, shrink = refs[m + 6 :]
    else:
        acc, best, kvs, s_buf, top, p_buf, shrink = refs[m + 2 :]
    z = place[2]
    count = 0
    for shift in shifts:
        count = count + jnp.where(z >= shift % 8, 1, 0)

    def source(b):
        shift = jnp.int32(shifts[-1])
        for k in range(n - 1):
            shift = jnp.where(b == k, shifts[k], shift)
        return lax.rem(z - shift + 8, 8)

    @pl.when(count > 0)
    def _():
        for k, ref in enumerate(blocks):
            kvs[k] = ref[...]

        run_items(
            4,
            count,
            lambda i: i,
            source,
            lambda i: 0,
            None,
            q, kvs, bias, acc, best, s_buf, top, p_buf, shrink,
        )

    if last:
        for slot in range(4):
            stats = []
            for h in range(2):
                total = acc[slot, h, 64:65, :]
                total = jnp.where(total > 0.0, total, 1.0)
                outs[slot][h * HEAD : (h + 1) * HEAD, :] = (
                    acc[slot, h, :HEAD, :] / total
                ).astype(BF16)
                log_sum = best[slot, h] + jnp.log2(total)
                hi = log_sum.astype(BF16).astype(F32)
                mid = (log_sum - hi).astype(BF16).astype(F32)
                low = log_sum - hi - mid
                stats += [hi, mid, low]
            stats.append(jnp.zeros((10, 512), F32))
            outs[slot][128:144, :] = jnp.concatenate(stats, axis=0).astype(BF16)


def attend_first(place, qs, kv, bias):
    return kernel(
        first_body, STATE + (shape(4, 128, 512),), (place, *qs, kv, bias), attend_scratch(1)
    )


def attend_more(place, q, bias, kvs, shifts, state, last=False):
    def body(*refs):
        more_body(shifts, last, *refs)

    n = len(kvs)
    outs = (shape(144, 512),) * 4 if last else ()
    aliases = {3 + n: len(outs), 4 + n: len(outs) + 1}
    scratch = attend_scratch(len(shifts))
    return kernel(body, outs + STATE, (place, q, bias, *kvs, *state), scratch, aliases)


def merge_body(place, own, r1, r2, r3, cum, log_out, *refs):
    pieces, rows = refs[:4], refs[4]
    y = place[0]
    parts = (own, r1, r2, r3)
    for h in range(2):
        logs = []
        for part in parts:
            stats = part[128:144, :].astype(F32)
            logs.append(
                stats[3 * h : 3 * h + 1] + stats[3 * h + 1 : 3 * h + 2] + stats[3 * h + 2 : 3 * h + 3]
            )
        peak = jnp.maximum(jnp.maximum(logs[0], logs[1]), jnp.maximum(logs[2], logs[3]))
        ws = [jnp.exp2(v - peak) for v in logs]
        total = ws[0] + ws[1] + ws[2] + ws[3]
        o = jnp.zeros((HEAD, 512), F32)
        for part, w in zip(parts, ws):
            o = o + part[h * HEAD : (h + 1) * HEAD, :].astype(F32) * w
        rows[:, h * HEAD : (h + 1) * HEAD] = jnp.transpose(o / total)
        log_out[h : h + 1, :] = (peak + jnp.log2(total)) * LN2 + cum[h : h + 1, :]
    for k in range(4):
        at = pl.multiple_of(lax.rem(y + k, 4) * 128, 128)
        pieces[k][...] = rows[pl.ds(at, 128), :].astype(BF16)


def per_device(
    tokens,
    norm_gain,
    w_query,
    w_key,
    w_value,
    conv_in,
    conv_gate,
    conv_taps,
    conv_gain,
    cum_gate,
    out_attn,
    out_conv,
):
    z = lax.axis_index("z")
    x = lax.axis_index("x")
    y = lax.axis_index("y")
    c = lax.axis_index("c")
    place = jnp.stack([y, c, z, x]).astype(jnp.int32)

    n0 = kernel(
        norm_body,
        shape(64, 2048),
        (tokens, norm_gain[None, :]),
        [
            pltpu.VMEM((64, 2048), BF16),
            pltpu.VMEM((1, 2048), F32),
            pltpu.SemaphoreType.DMA((2,)),
        ],
        scalars=0,
        far=2,
    )
    own = [n0] + [turn(n0, "y", k) for k in (1, 2, 3)]
    partner = [turn(piece, "c", 1) for piece in own]

    ws = [out_attn] + [turn(out_attn, "y", k) for k in (1, 2, 3)]

    bias, cum_own = kernel(
        bias_body, (shape(8, 512, 128), shape(2, 512, dtype=F32)), (place, cum_gate)
    )
    weights = kernel(
        load_body,
        shape(2048, 896),
        (cum_own, w_query, w_key, w_value, conv_in, conv_gate),
        [pltpu.SemaphoreType.DMA((5,))],
        scalars=0,
        far=5,
    )

    qT, kv, gated, rim = kernel(
        project_body,
        (shape(128, 512), shape(1024, 128), shape(512, 256), shape(32, 256)),
        (place, *own, *partner, weights),
        [pltpu.VMEM((512, 2048), BF16)],
    )

    rim = lax.ppermute(rim, ("z", "x"), [(i, i + 1) for i in range(31)])
    a1 = turn(kv, "z", 1)
    b1 = turn(kv, "z", -1)
    qs = [qT] + [turn(qT, "x", k) for k in (1, 2, 3)]
    a2 = turn(a1, "z", 1)
    b2 = turn(b1, "z", -1)
    a3 = turn(a2, "z", 1)
    b3 = turn(b2, "z", -1)
    a4 = turn(a3, "z", 1)

    convolved, square = kernel(
        conv_body,
        (shape(512, 256, dtype=F32), shape(1, 512, dtype=F32)),
        (gated, rim, conv_taps),
        [pltpu.VMEM((8, 544, 256), F32)],
        scalars=0,
    )
    square = square + turn(square, "c", 1)
    square = square + swap(square, "y", 1)
    square = square + swap(square, "y", 2)
    parts = kernel(
        gate_body,
        (shape(128, 2048),) * 4,
        (place, convolved, square, conv_gain[None, :], out_conv),
        [pltpu.VMEM((512, 256), BF16)],
    )
    parts = [parts[0]] + [turn(parts[k], "y", k) for k in (1, 2, 3)]

    *state, q = attend_first(place, qs, kv, bias)
    state = attend_more(place, q, bias, (a1, b1), (1, -1), state)
    state = attend_more(place, q, bias, (a2, b2), (2, -2), state)
    outs = attend_more(place, q, bias, (a3, a4, b3), (3, 4, -3), state, True)
    others = [turn(outs[k], "x", -k) for k in (1, 2, 3)]
    log_total, *pieces = kernel(
        merge_body,
        (shape(2, 512, dtype=F32),) + (shape(128, 128),) * 4,
        (place, outs[0], *others, cum_own),
        [pltpu.VMEM((512, 128), F32)],
    )
    heads = [pieces[0]] + [turn(pieces[k], "y", k) for k in (1, 2, 3)]
    mine, theirs = kernel(
        part_body,
        (shape(64, 2048, dtype=F32), shape(64, 2048)),
        (place, *heads, *parts, *ws),
        [pltpu.VMEM((128, 2048), F32)],
    )
    theirs = turn(theirs, "c", 1)
    mixed = kernel(final_body, shape(64, 2048), (mine, theirs), scalars=0)
    return (mixed, log_total)


def solution(mesh):
    grid = Mesh(mesh.devices.reshape(8, 4, 4, 2), ("z", "x", "y", "c"))
    sp = ("z", "x")
    tp = ("y", "c")
    in_specs = (
        P(sp + tp, None),
        P(),
        P(None, tp),
        P(None, tp),
        P(None, tp),
        P(None, tp),
        P(None, tp),
        P(None, tp),
        P(tp),
        P(tp, None),
        P(tp, None),
        P(tp, None),
    )
    out_specs = (P(sp + tp, None), P(tp, sp))

    return jax.shard_map(
        per_device, mesh=grid, in_specs=in_specs, out_specs=out_specs, check_vma=False
    )
```
